32 devices in a mesh: ep: 8 (over z, x), tp: 4 (over y, core).
Axes of the slice: x: 2, y: 2, z: 4, core: 2. Of those that a mesh axis runs over, the one named last changes fastest.
Arguments:
- queries: bfloat16 [2048, 1024], P('ep', 'tp'), may hold values from -192 to 192
- keys_values: bfloat16 [2048, 512], P('ep', 'tp'), may hold values from -192 to 192
- log_gate_cum: float32 [16, 2048], P('tp'), as said below
- mix_weight: bfloat16 [1024, 2048], P('tp'), may hold values from -0.1875 to 0.1875
- mix_gain: float32 [2048], replicated, may hold values from 0.1 to 1.9
- moe_in: bfloat16 [6144, 2048], P(('ep', 'tp')), may hold values from -6 to 6
- moe_gain: float32 [2048], replicated, may hold values from 0.1 to 1.9
- routes: int32 [6144, 2], P(('ep', 'tp')), may hold values from 0 to 7, all different within a row; in each aligned block of 192 rows (0 to 191, 192 to 383, ...) at most 72 rows name the same one
- route_weight: float32 [6144, 2], P(('ep', 'tp')), may hold values from 0.25 to 2
- expert_gate: bfloat16 [8, 2048, 1024], P('ep', None, 'tp'), may hold values from -0.125 to 0.125
- expert_up: bfloat16 [8, 2048, 1024], P('ep', None, 'tp'), may hold values from -0.125 to 0.125
- expert_down: bfloat16 [8, 1024, 2048], P('ep', 'tp'), may hold values from -0.1875 to 0.1875
Outputs:
- mix_result: bfloat16 [2048, 2048], P(('ep', 'tp'))
- moe_result: bfloat16 [6144, 2048], P(('ep', 'tp'))
The draws below stay inside these ranges and needn't reach their ends.
Inputs may be any that keep to these rules, and one draw needn't show every extreme that they name: `log_gate_cum`: along positions each head's values never rise. `routes`: each row names 2 different experts. Among the rows of one device no expert is named more than 72 times, and in every draw some device names some expert exactly 72 times.
All inputs are finite; a program needn't handle non-finite values.
Results may differ from the reference program's by a relative error of at most 0.013.
Values may be sent and summed in bfloat16 or wider, within the bound.
A program may use at most 128 MiB of HBM per device.

```python
import math
import jax
import jax.numpy as jnp
import numpy as np
from jax import lax

D = 2048
ASKING_ATTENDERS = 16
KV_HEADS = 4
HEAD = 64
FF = 1024
TOPK = 2
TOK_EP = 256
TOK_M = 192
CONTEXT_SPAN = 2048
EXPERTS = 8
CAP = 72
TOKENS_M = 6144
N_EP = 8
N_TP = 4


def attention_pair(key):
    queries = jnp.clip(jax.random.normal(jax.random.fold_in(key, 31), (CONTEXT_SPAN, ASKING_ATTENDERS * HEAD), jnp.float32), -4.5, 4.5)
    paired = jnp.clip(jax.random.normal(jax.random.fold_in(key, 32), (CONTEXT_SPAN, KV_HEADS, 2, HEAD), jnp.float32), -4.5, 4.5)
    return (queries, paired.reshape(CONTEXT_SPAN, KV_HEADS * 2 * HEAD))


def draw_queries(key, part):
    return attention_pair(key)[0].astype(jnp.bfloat16)


def draw_keys_values(key, part):
    return attention_pair(key)[1].astype(jnp.bfloat16)


def draw_log_gate_cum(key, part):
    attender_ordinal = jnp.arange(ASKING_ATTENDERS, dtype=jnp.int32)
    ranking = jax.random.permutation(jax.random.fold_in(key, 41), ASKING_ATTENDERS)
    fast_count = ASKING_ATTENDERS // 2
    is_fast = ranking < fast_count
    fast_rate = jnp.exp(jax.random.uniform(jax.random.fold_in(key, 42), (ASKING_ATTENDERS,), jnp.float32, math.log(0.01), math.log(1.0 / 30.0)))
    slow_rate = jnp.exp(jax.random.uniform(jax.random.fold_in(key, 43), (ASKING_ATTENDERS,), jnp.float32, math.log(0.3), 0.0)) / CONTEXT_SPAN
    rate = jnp.where(is_fast, fast_rate, slow_rate)[:, None]
    block_factor = jnp.exp(jax.random.uniform(jax.random.fold_in(key, 44), (ASKING_ATTENDERS, N_EP), jnp.float32, math.log(0.5), math.log(2.0)))
    block_factor = jnp.repeat(block_factor, TOK_EP, axis=1)
    roughness = jax.random.uniform(jax.random.fold_in(key, 45), (ASKING_ATTENDERS, CONTEXT_SPAN), jnp.float32, 0.3, 1.7)
    doubling_rounds = -rate * block_factor * roughness
    span_offset = jax.random.randint(jax.random.fold_in(key, 46), (ASKING_ATTENDERS, 3), 0, CONTEXT_SPAN)
    span_extent = jax.random.uniform(jax.random.fold_in(key, 47), (ASKING_ATTENDERS, 3), jnp.float32, 0.22, 0.5)
    doubling_rounds = doubling_rounds.at[attender_ordinal[:, None], span_offset].add(-span_extent)
    return jnp.cumsum(doubling_rounds, axis=1)


def steps_of(key, dims, shards, low, top_value):
    factor_of, own = 1.0, jax.random.fold_in(key, 6)
    for position, shards_of in shards:
        heights = jnp.exp(jax.random.uniform(jax.random.fold_in(own, position), (shards_of,), jnp.float32, low / len(shards), top_value / len(shards)))
        factor_of = factor_of * jnp.repeat(heights, dims[position] // shards_of).reshape([-1 if axis == position else 1 for axis in range(len(dims))])
    return factor_of


def assign_block(stream_key, own, number, rows, amount, top, most, slope):
    order = jax.random.permutation(stream_key, amount)
    crowded, ordinary = shares(amount, rows * top, most, slope, True), shares(amount, rows * top, most, slope, False)
    places = jnp.arange(amount)

    def named(sizes, turn):
        used = int((sizes > 0).sum())
        fixed = max(1, used // 4)
        shifted = fixed + (places - fixed + turn * (used - fixed)) % max(1, amount - fixed)
        return jnp.zeros((amount,), jnp.int32).at[order[jnp.where(places < fixed, places, shifted)]].set(jnp.asarray(sizes, jnp.int32))

    sizes = jnp.where(number % 4 == 0, named(crowded, number // 4), named(ordinary, number - number // 4 - 1))
    mixed = jax.random.permutation(jax.random.fold_in(own, 3), amount)
    source_of, sink = mixed[0:amount // 2 * 2:2], mixed[1:amount // 2 * 2:2]
    margin = jnp.minimum(sizes[source_of] - 1, most - sizes[sink]) // 2
    margin = jnp.where((source_of == order[0]) | (sink == order[0]) | (sizes[sink] == 0), 0, jnp.maximum(margin, 0))
    shifted = jax.random.randint(jax.random.fold_in(own, 4), (amount // 2,), 0, 1 << 20) % (margin + 1)
    sizes = sizes.at[source_of].add(-shifted).at[sink].add(shifted)
    items = jnp.searchsorted(jnp.cumsum(sizes), jnp.arange(rows * top), side="right").astype(jnp.int32)
    grid = items.reshape(top, rows).T
    grid = grid[jax.random.permutation(jax.random.fold_in(own, 1), rows)]
    turn = jax.random.randint(jax.random.fold_in(own, 2), (rows, 1), 0, top)
    return jnp.take_along_axis(grid, (jnp.arange(top)[None, :] + turn) % top, axis=1)


def shares(number_of, total, limit, slope, full):
    weights = [(1 << 20) // math.isqrt(grade ** slope) + 1 for grade in range(1, number_of + 1)]
    largest = limit if full else min(limit, max(-(-total // number_of), total * weights[0] // sum(weights)))
    least = 1 if total - largest >= number_of - 1 else 0
    given, spare = [largest] + [least] * (number_of - 1), total - largest - least * (number_of - 1)
    while spare > 0:
        movable = [i for i in range(1, number_of) if given[i] < largest] or [i for i in range(1, number_of) if given[i] < limit]
        pool, budget = sum([weights[i] for i in movable]), spare
        for i in movable:
            extra = min(limit - given[i], max(1, budget * weights[i] // pool), spare)
            given[i] = given[i] + extra
            spare = spare - extra
    return np.array(given)


def gaussian(rng, shape, deviation, limit, pieces=(), kind=jnp.bfloat16):
    values = deviation * jax.random.normal(rng, shape, jnp.float32)
    if pieces:
        values = values * steps_of(rng, shape, pieces, -0.22, 0.18)
    return jnp.clip(values, -limit, limit).astype(kind)


def setup_inputs(seed: int = 0) -> dict:
    seeds = jax.random.split(jax.random.key(seed), 13)
    queries = draw_queries(jax.random.fold_in(seeds[12], 71), 0)
    keys_values = draw_keys_values(jax.random.fold_in(seeds[12], 71), 0)
    log_gate_cum = draw_log_gate_cum(jax.random.fold_in(seeds[12], 71), 0)
    mix_weight = gaussian(seeds[3], (ASKING_ATTENDERS * HEAD, D), (ASKING_ATTENDERS * HEAD) ** -0.5, 0.1875, ((0, 4),))
    mix_gain = jnp.clip(1.0 + 0.18 * jax.random.normal(seeds[4], (D,), jnp.float32), 0.1, 1.9)
    moe_in = gaussian(seeds[5], (TOKENS_M, D), 1.0, 6.0, ((0, 32),))
    moe_gain = jnp.clip(1.0 + 0.18 * jax.random.normal(seeds[6], (D,), jnp.float32), 0.1, 1.9)
    routes_keys = jax.random.split(jax.random.fold_in(seeds[7], 1), TOKENS_M // TOK_M)
    routes_turns = jax.random.permutation(jax.random.fold_in(seeds[7], 3), TOKENS_M // TOK_M)
    routes = jax.vmap(lambda own, number: assign_block(jax.random.fold_in(seeds[7], 2), own, number, TOK_M, EXPERTS, TOPK, CAP, 2))(routes_keys, routes_turns).reshape((TOKENS_M, TOPK))
    route_weight = jnp.clip(jnp.exp(math.log(2.0) - 2.0794415 * jax.random.uniform(seeds[8], (TOKENS_M, TOPK), jnp.float32) ** steps_of(seeds[8], (TOKENS_M, TOPK), ((0, 32),), -0.2, 0.2)), 0.25, 2.0)
    expert_gate = gaussian(seeds[9], (EXPERTS, D, FF), D ** -0.5, 0.125, ((0, 8), (2, 4)))
    expert_up = gaussian(seeds[10], (EXPERTS, D, FF), D ** -0.5, 0.125, ((0, 8), (2, 4)))
    expert_down = gaussian(seeds[11], (EXPERTS, FF, D), FF ** -0.5, 0.1875, ((0, 8), (1, 4)))
    return dict(queries=queries, keys_values=keys_values, log_gate_cum=log_gate_cum, mix_weight=mix_weight, mix_gain=mix_gain, moe_in=moe_in, moe_gain=moe_gain, routes=routes, route_weight=route_weight, expert_gate=expert_gate, expert_up=expert_up, expert_down=expert_down)


EPSILON = 1e-06

def rms_scale(values, gain):
    widened = values.astype(jnp.float32)
    return widened * lax.rsqrt(lax.optimization_barrier(jnp.mean(widened * widened, axis=-1, keepdims=True)) + EPSILON) * gain

def attend_reference(queries, keys_values, log_gate_cum):
    seq_len = queries.shape[0]
    group_size = ASKING_ATTENDERS // KV_HEADS
    block_rows = math.gcd(seq_len, 256)
    paired = keys_values.reshape(seq_len, KV_HEADS, 2, HEAD).astype(jnp.float32)
    key_part = paired[:, :, 0]
    value_part = paired[:, :, 1]
    gates = log_gate_cum.reshape(KV_HEADS, group_size, seq_len)
    key_pos = jnp.arange(seq_len, dtype=jnp.int32)

    def one_block(block_index):
        first_row = block_index * block_rows
        query_block = lax.dynamic_slice_in_dim(queries, first_row, block_rows, 0)
        query_block = query_block.reshape(block_rows, KV_HEADS, group_size, HEAD).astype(jnp.float32)
        scores = jnp.einsum('tgrd,ngd->grtn', query_block, key_part) * HEAD ** (-0.5)
        query_gate = lax.dynamic_slice_in_dim(gates, first_row, block_rows, 2)
        scores = scores + query_gate[..., None] - gates[:, :, None, :]
        query_pos = first_row + jnp.arange(block_rows, dtype=jnp.int32)
        causal = key_pos[None, :] <= query_pos[:, None]
        scores = jnp.where(causal, scores, -jnp.inf)
        row_max = lax.optimization_barrier(jnp.max(scores, axis=-1, keepdims=True))
        weight = jnp.exp(scores - row_max)
        row_total = lax.optimization_barrier(jnp.sum(weight, axis=-1))
        weight_b = lax.optimization_barrier(weight.astype(jnp.bfloat16)).astype(jnp.float32)
        mixed_heads = jnp.einsum('grtn,ngd->grtd', weight_b, value_part) / row_total[..., None]
        mixed_heads = jnp.transpose(mixed_heads, (2, 0, 1, 3)).reshape(block_rows, ASKING_ATTENDERS * HEAD)
        return mixed_heads.astype(jnp.bfloat16)
    blocks = lax.map(one_block, jnp.arange(seq_len // block_rows, dtype=jnp.int32))
    return blocks.reshape(seq_len, ASKING_ATTENDERS * HEAD)

def reference(queries, keys_values, log_gate_cum, mix_weight, mix_gain, moe_in, moe_gain, routes, route_weight, expert_gate, expert_up, expert_down):
    attended = attend_reference(queries, keys_values, log_gate_cum)
    seq_len = attended.shape[0]
    head_width = ASKING_ATTENDERS * HEAD // N_TP
    projected = jnp.zeros((seq_len, D), jnp.float32)
    for shard_index in range(N_TP):
        head_part = jnp.dot(attended[:, shard_index * head_width:(shard_index + 1) * head_width], mix_weight[shard_index * head_width:(shard_index + 1) * head_width], preferred_element_type=jnp.float32).astype(jnp.bfloat16)
        projected = projected + lax.optimization_barrier(head_part).astype(jnp.float32)
    mix_result = rms_scale(projected, mix_gain).astype(jnp.bfloat16)
    normed = rms_scale(moe_in, moe_gain).astype(jnp.bfloat16)
    token_count = normed.shape[0]
    flat_routes = routes.reshape(-1).astype(jnp.int32)
    flat_weight = route_weight.reshape(-1)
    order = jnp.argsort(flat_routes, stable=True).astype(jnp.int32)
    most_rows = N_EP * N_TP * CAP
    expert_ids = jnp.arange(EXPERTS, dtype=jnp.int32)
    counts = lax.optimization_barrier(jnp.sum((flat_routes[:, None] == expert_ids[None, :]).astype(jnp.int32), axis=0))
    starts = (jnp.cumsum(counts) - counts).astype(jnp.int32)
    order_padded = jnp.concatenate([order, jnp.zeros((most_rows,), jnp.int32)])
    ff_width = FF // N_TP

    def one_expert(accum, inputs):
        gate_here, up_here, down_here, first_slot, count_here = inputs
        picked = lax.dynamic_slice_in_dim(order_padded, first_slot, most_rows, 0)
        valid = jnp.arange(most_rows, dtype=jnp.int32) < count_here
        token_ids = (picked // TOPK).astype(jnp.int32)
        rows_in = normed[token_ids]
        hidden = (jax.nn.silu(jnp.dot(rows_in, gate_here, preferred_element_type=jnp.float32)) * jnp.dot(rows_in, up_here, preferred_element_type=jnp.float32)).astype(jnp.bfloat16)
        summed = jnp.zeros((most_rows, D), jnp.float32)
        for shard_index in range(N_TP):
            width_part = jnp.dot(hidden[:, shard_index * ff_width:(shard_index + 1) * ff_width], down_here[shard_index * ff_width:(shard_index + 1) * ff_width], preferred_element_type=jnp.float32).astype(jnp.bfloat16)
            summed = summed + lax.optimization_barrier(width_part).astype(jnp.float32)
        expert_out = lax.optimization_barrier(summed.astype(jnp.bfloat16)).astype(jnp.float32)
        scaled = jnp.where(valid, flat_weight[picked], 0.0)
        accum = accum.at[token_ids].add(scaled[:, None] * expert_out)
        return (accum, None)
    accum, _ = lax.scan(one_expert, jnp.zeros((token_count, D), jnp.float32), (expert_gate, expert_up, expert_down, starts, counts))
    moe_result = accum.astype(jnp.bfloat16)
    return (mix_result, moe_result)
```

```python
from functools import partial

import jax
import jax.numpy as jnp
from jax import lax
from jax.experimental import pallas as pl
from jax.experimental.pallas import tpu as pltpu
from jax.sharding import PartitionSpec as P

HEAD = 64
EPSILON = 1e-06
NEGATIVE = -1e30
MESH = pl.DeviceIdType.MESH
F32 = jnp.float32
BF16 = jnp.bfloat16


def round_up(value, unit):
    return -(-value // unit) * unit


def dot(a, b):
    return jnp.dot(a, b, preferred_element_type=F32)


def iota(shape, dim):
    return lax.broadcasted_iota(jnp.int32, shape, dim)


def rms_scale(widened, gain):
    return widened * lax.rsqrt(jnp.mean(widened * widened, axis=-1, keepdims=True) + EPSILON) * gain


def kernel(
    sizes,
    q_ref,
    kv_ref,
    key_gate_ref,
    query_gate_ref,
    mixw_ref,
    mix_gain_ref,
    x_ref,
    x_gain_ref,
    routes_ref,
    routes_t_ref,
    route_weight_ref,
    gate_hbm,
    up_hbm,
    down_hbm,
    mix_out,
    moe_out,
    gate_all,
    up_all,
    down_all,
    send_x,
    recv_x,
    hidden,
    send_y,
    recv_y,
    kv_all,
    q_pad,
    top,
    total,
    summed,
    mix_send,
    mix_recv,
    local_sem,
    far_send,
    far_recv,
    own_send,
    own_recv,
    fwd_send,
    fwd_recv,
    x_send_sem,
    x_recv_sem,
    kv_send_sem,
    kv_recv_sem,
    y_send_sem,
    y_recv_sem,
    mix_send_sem,
    mix_recv_sem,
):
    ep, tp, slot_rows, wire_rows, chunks = sizes
    me = lax.axis_index("ep")
    tme = lax.axis_index("tp")
    far = lax.rem(tme + tp // 2, tp)
    near = tme + 1 - 2 * lax.rem(tme, 2)
    near_far = lax.rem(near + tp // 2, tp)
    rows, width = x_ref.shape
    picks = routes_ref.shape[1]
    slots = ep * slot_rows
    shard = down_hbm.shape[1]
    cols = width // chunks
    tokens = q_ref.shape[0]
    heads = query_gate_ref.shape[1]
    kv_local = kv_ref.shape[1] // (2 * HEAD)
    group = heads // kv_local

    def weight_view(item, block):
        if item == 0:
            return gate_all.at[block]
        if item == 1:
            return up_all.at[block]
        return down_all.at[item - 2, pl.ds(pl.multiple_of(block * shard, shard), shard)]

    def weight_source(item):
        if item == 0:
            return gate_hbm.at[0]
        if item == 1:
            return up_hbm.at[0]
        return down_hbm.at[0, :, pl.ds((item - 2) * cols, cols)]

    items = 2 + chunks
    loads = [
        pltpu.make_async_copy(weight_source(i), weight_view(i, tme), local_sem.at[i])
        for i in range(items)
    ]
    for load in loads:
        load.start()
    recv_x[...] = jnp.zeros_like(recv_x)
    recv_y[...] = jnp.zeros_like(recv_y)

    barrier = pltpu.get_barrier_semaphore()

    def greet(step, carry):
        pl.semaphore_signal(
            barrier, inc=1, device_id={"ep": lax.rem(me + step, ep)}, device_id_type=MESH
        )
        return carry

    lax.fori_loop(1, ep, greet, 0)
    for step in range(1, tp):
        pl.semaphore_signal(
            barrier, inc=1, device_id={"tp": lax.rem(tme + step, tp)}, device_id_type=MESH
        )
    pl.semaphore_wait(barrier, ep - 1 + tp - 1)

    def weight_copy(item, block, target, send_sem, recv_sem):
        view = weight_view(item, block)
        return pltpu.make_async_remote_copy(
            src_ref=view,
            dst_ref=view,
            send_sem=send_sem.at[item],
            recv_sem=recv_sem.at[item],
            device_id={"tp": target},
            device_id_type=MESH,
        )

    far_copies, own_copies, fwd_copies = [], [], []
    for i in range(items):
        loads[i].wait()
        far_copies.append(weight_copy(i, tme, far, far_send, far_recv))
        far_copies[i].start()
        own_copies.append(weight_copy(i, tme, near, own_send, own_recv))
        own_copies[i].start()
        fwd_copies.append(weight_copy(i, far, near, fwd_send, fwd_recv))

    def far_arrival(item):
        return weight_copy(item, far, far, far_send, far_recv)

    def near_arrival(item):
        return weight_copy(item, near, near, own_send, own_recv)

    def near_far_arrival(item):
        return weight_copy(item, near_far, near, fwd_send, fwd_recv)

    normed = rms_scale(x_ref[...].astype(F32), x_gain_ref[...]).astype(BF16)
    expert_row = iota((ep, rows), 0)
    named_t = jnp.zeros((ep, rows), F32)
    for k in range(picks):
        named_t = named_t + jnp.where(routes_t_ref[k : k + 1, :] == expert_row, 1.0, 0.0)
    before_t = jnp.where(iota((rows, rows), 0) < iota((rows, rows), 1), 1.0, 0.0).astype(BF16)
    place_t = dot(named_t.astype(BF16), before_t) + (expert_row * slot_rows).astype(F32)
    slot_iota = iota((slots, rows), 0)
    pick_t = jnp.zeros((slots, rows), F32)
    for k in range(picks):
        slot_t = jnp.sum(
            jnp.where(routes_t_ref[k : k + 1, :] == expert_row, place_t, 0.0), axis=0, keepdims=True
        ).astype(jnp.int32)
        pick_t = pick_t + jnp.where(slot_iota == slot_t, 1.0, 0.0)
    pick_t = pick_t.astype(BF16)
    for c in range(chunks):
        send_x[:, :, c * cols : (c + 1) * cols] = (
            dot(pick_t, normed[:, c * cols : (c + 1) * cols])
            .astype(BF16)
            .reshape(ep, slot_rows, cols)
        )

    def x_copy(target, source):
        return pltpu.make_async_remote_copy(
            src_ref=send_x.at[target, pl.ds(0, wire_rows)],
            dst_ref=recv_x.at[source, pl.ds(0, wire_rows)],
            send_sem=x_send_sem.at[target],
            recv_sem=x_recv_sem.at[source],
            device_id={"ep": target},
            device_id_type=MESH,
        )

    def kv_copy(target, source):
        return pltpu.make_async_remote_copy(
            src_ref=kv_ref,
            dst_ref=kv_all.at[source],
            send_sem=kv_send_sem.at[target],
            recv_sem=kv_recv_sem.at[source],
            device_id={"ep": target},
            device_id_type=MESH,
        )

    def over_peers(action):
        def step_of(step, carry):
            action(lax.rem(me + step, ep))
            return carry

        lax.fori_loop(1, ep, step_of, 0)

    over_peers(lambda peer: x_copy(peer, me).start())

    def kv_start(peer, carry):
        kv_copy(peer, me).start()
        return carry

    lax.fori_loop(me + 1, ep, kv_start, 0)
    recv_x[me] = send_x[me]
    kv_all[me] = kv_ref[...]

    expert_col = iota((rows, ep), 1)
    named = jnp.zeros((rows, ep), F32)
    for k in range(picks):
        named = named + jnp.where(routes_ref[:, k : k + 1] == expert_col, 1.0, 0.0)
    before = jnp.where(iota((rows, rows), 0) > iota((rows, rows), 1), 1.0, 0.0).astype(BF16)
    place = dot(before, named.astype(BF16)) + (expert_col * slot_rows).astype(F32)
    slot_of = [
        jnp.sum(
            jnp.where(routes_ref[:, k : k + 1] == expert_col, place, 0.0), axis=1, keepdims=True
        ).astype(jnp.int32)
        for k in range(picks)
    ]
    for h in range(heads):
        select = jnp.where(
            (iota((heads * HEAD, 2 * HEAD), 0) == iota((heads * HEAD, 2 * HEAD), 1) + h * HEAD)
            & (iota((heads * HEAD, 2 * HEAD), 1) < HEAD),
            1.0,
            0.0,
        ).astype(BF16)
        q_pad[h] = dot(q_ref[...], select).astype(BF16)
    top[...] = jnp.full(top.shape, NEGATIVE, F32)
    total[...] = jnp.zeros_like(total)
    summed[...] = jnp.zeros_like(summed)

    for i in range(2):
        far_arrival(i).wait_recv()
        fwd_copies[i].start()
    for i in range(2):
        near_arrival(i).wait_recv()
        near_far_arrival(i).wait_recv()
    over_peers(lambda peer: x_copy(me, peer).wait_recv())

    def hidden_block(block, carry):
        taken = recv_x[...].reshape(slots, width)
        gated = dot(taken, gate_all[block])
        lifted = dot(taken, up_all[block])
        hidden[:, pl.ds(pl.multiple_of(block * shard, shard), shard)] = (
            gated / (1.0 + jnp.exp(-gated)) * lifted
        ).astype(BF16)
        return carry

    lax.fori_loop(0, tp, hidden_block, 0)
    for i in range(2, items):
        far_arrival(i).wait_recv()
        fwd_copies[i].start()

    def y_copy(c, target, source):
        return pltpu.make_async_remote_copy(
            src_ref=send_y.at[c, target, pl.ds(0, wire_rows)],
            dst_ref=recv_y.at[c, source, pl.ds(0, wire_rows)],
            send_sem=y_send_sem.at[c, target],
            recv_sem=y_recv_sem.at[c, source],
            device_id={"ep": target},
            device_id_type=MESH,
        )

    for c in range(chunks):
        near_arrival(2 + c).wait_recv()
        near_far_arrival(2 + c).wait_recv()
        send_y[c] = dot(hidden[...], down_all[c]).astype(BF16).reshape(ep, slot_rows, cols)
        over_peers(lambda peer: y_copy(c, peer, me).start())
        recv_y[c, me] = send_y[c, me]

    def key_block(block, carry):
        @pl.when(block < me)
        def _():
            kv_copy(me, block).wait_recv()

        causal = block * tokens + iota((tokens, tokens), 1) <= me * tokens + iota(
            (tokens, tokens), 0
        )
        for h in range(heads):
            pair = kv_all[block, :, (h // group) * 2 * HEAD : (h // group + 1) * 2 * HEAD]
            scores = (
                lax.dot_general(
                    q_pad[h], pair, (((1,), (1,)), ((), ())), preferred_element_type=F32
                )
                * HEAD ** (-0.5)
            )
            scores = scores + query_gate_ref[:, h : h + 1] - key_gate_ref[block, h : h + 1, :]
            scores = jnp.where(causal, scores, NEGATIVE)
            old = top[h]
            new = jnp.maximum(old, jnp.max(scores, axis=-1, keepdims=True))
            factor = jnp.exp(old - new)
            weight = jnp.where(causal, jnp.exp(scores - new[:, :1]), 0.0)
            top[h] = new
            total[h] = total[h] * factor + jnp.sum(weight, axis=-1, keepdims=True)
            summed[h] = summed[h] * factor + dot(weight.astype(BF16), pair)
        return carry

    lax.fori_loop(0, me + 1, key_block, 0)
    attended = jnp.zeros((tokens, heads * HEAD), F32)
    for h in range(heads):
        part = (summed[h] / total[h]).astype(BF16)
        select = jnp.where(
            (iota((2 * HEAD, heads * HEAD), 0) + (h - 1) * HEAD == iota((2 * HEAD, heads * HEAD), 1))
            & (iota((2 * HEAD, heads * HEAD), 0) >= HEAD),
            1.0,
            0.0,
        ).astype(BF16)
        attended = attended + dot(part, select)
    attended = attended.astype(BF16)
    for c in range(chunks):
        mix_send[:, :, c * cols : (c + 1) * cols] = (
            dot(attended, mixw_ref[:, c * cols : (c + 1) * cols])
            .astype(BF16)
            .reshape(tp, tokens // tp, cols)
        )

    def mix_copy(target, source):
        return pltpu.make_async_remote_copy(
            src_ref=mix_send.at[target],
            dst_ref=mix_recv.at[source],
            send_sem=mix_send_sem.at[target],
            recv_sem=mix_recv_sem.at[source],
            device_id={"tp": target},
            device_id_type=MESH,
        )

    for step in range(1, tp):
        mix_copy(lax.rem(tme + step, tp), tme).start()
    mix_recv[tme] = mix_send[tme]
    for step in range(1, tp):
        mix_copy(tme, lax.rem(tme + step, tp)).wait_recv()
    mixed = mix_recv[0].astype(F32)
    for j in range(1, tp):
        mixed = mixed + mix_recv[j].astype(F32)
    mix_out[...] = rms_scale(mixed, mix_gain_ref[...]).astype(BF16)

    slot_lane = iota((rows, slots), 1)
    for c in range(chunks):
        over_peers(lambda peer: y_copy(c, me, peer).wait_recv())
        back = recv_y[c].reshape(slots, cols)
        blend = jnp.zeros((rows, cols), F32)
        for k in range(picks):
            pick = jnp.where(slot_lane == slot_of[k], 1.0, 0.0).astype(BF16)
            blend = blend + route_weight_ref[:, k : k + 1] * dot(pick, back)
        moe_out[:, c * cols : (c + 1) * cols] = blend.astype(BF16)

    for i in range(items):
        far_copies[i].wait_send()
        own_copies[i].wait_send()
        fwd_copies[i].wait_send()
    over_peers(lambda peer: x_copy(peer, me).wait_send())

    def kv_end(peer, carry):
        kv_copy(peer, me).wait_send()
        return carry

    lax.fori_loop(me + 1, ep, kv_end, 0)
    for c in range(chunks):
        over_peers(lambda peer: y_copy(c, peer, me).wait_send())
    for step in range(1, tp):
        mix_copy(lax.rem(tme + step, tp), tme).wait_send()


def body(
    queries,
    keys_values,
    log_gate_cum,
    mix_weight,
    mix_gain,
    moe_in,
    moe_gain,
    routes,
    route_weight,
    expert_gate,
    expert_up,
    expert_down,
):
    ep, tp = lax.axis_size("ep"), lax.axis_size("tp")
    me = lax.axis_index("ep")
    tokens = queries.shape[0]
    heads = log_gate_cum.shape[0]
    rows, width = moe_in.shape
    picks = routes.shape[1]
    capacity = 3 * picks * rows // (2 * ep)
    slot_rows, wire_rows = round_up(capacity, 16), round_up(capacity, WIRE)
    chunks = 4
    cols = width // chunks
    depth, shard = expert_gate.shape[1:]
    key_gate = jnp.transpose(log_gate_cum.reshape(heads, ep, tokens), (1, 0, 2))
    query_gate = lax.dynamic_slice_in_dim(log_gate_cum, me * tokens, tokens, 1).T
    vmem = pl.BlockSpec(memory_space=pltpu.VMEM)
    hbm = pl.BlockSpec(memory_space=pl.ANY)
    dma = pltpu.SemaphoreType.DMA
    items = 2 + chunks
    return pl.pallas_call(
        partial(kernel, (ep, tp, slot_rows, wire_rows, chunks)),
        out_shape=(
            jax.ShapeDtypeStruct((tokens // tp, width), BF16),
            jax.ShapeDtypeStruct((rows, width), BF16),
        ),
        in_specs=[vmem] * 11 + [hbm] * 3,
        out_specs=(vmem, vmem),
        scratch_shapes=[
            pltpu.VMEM((tp, depth, shard), BF16),
            pltpu.VMEM((tp, depth, shard), BF16),
            pltpu.VMEM((chunks, tp * shard, cols), BF16),
            pltpu.VMEM((ep, slot_rows, width), BF16),
            pltpu.VMEM((ep, slot_rows, width), BF16),
            pltpu.VMEM((ep * slot_rows, tp * shard), BF16),
            pltpu.VMEM((chunks, ep, slot_rows, cols), BF16),
            pltpu.VMEM((chunks, ep, slot_rows, cols), BF16),
            pltpu.VMEM((ep,) + keys_values.shape, BF16),
            pltpu.VMEM((heads, tokens, 2 * HEAD), BF16),
            pltpu.VMEM((heads, tokens, 2 * HEAD), F32),
            pltpu.VMEM((heads, tokens, 2 * HEAD), F32),
            pltpu.VMEM((heads, tokens, 2 * HEAD), F32),
            pltpu.VMEM((tp, tokens // tp, width), BF16),
            pltpu.VMEM((tp, tokens // tp, width), BF16),
        ]
        + [dma((items,))] * 7
        + [dma((ep,))] * 4
        + [dma((chunks, ep))] * 2
        + [dma((tp,))] * 2,
        compiler_params=pltpu.CompilerParams(
            collective_id=0, has_side_effects=True, vmem_limit_bytes=60 * 1024 * 1024
        ),
    )(
        queries,
        keys_values,
        key_gate,
        query_gate,
        mix_weight,
        mix_gain.reshape(1, -1),
        moe_in,
        moe_gain.reshape(1, -1),
        routes,
        routes.T,
        route_weight,
        expert_gate,
        expert_up,
        expert_down,
    )


WIRE = 8


def solution(mesh):
    in_specs = (
        P("ep", "tp"),
        P("ep", "tp"),
        P("tp", None),
        P("tp", None),
        P(),
        P(("ep", "tp"), None),
        P(),
        P(("ep", "tp"), None),
        P(("ep", "tp"), None),
        P("ep", None, "tp"),
        P("ep", None, "tp"),
        P("ep", "tp", None),
    )
    out_specs = (P(("ep", "tp"), None), P(("ep", "tp"), None))
    return jax.shard_map(body, mesh=mesh, in_specs=in_specs, out_specs=out_specs, check_vma=False)
```

```python
from functools import partial

import jax
import jax.numpy as jnp
from jax import lax
from jax.experimental import pallas as pl
from jax.experimental.pallas import tpu as pltpu
from jax.sharding import PartitionSpec as P

HEAD = 64
EPSILON = 1e-06
NEGATIVE = -1e30
MESH = pl.DeviceIdType.MESH
F32 = jnp.float32
BF16 = jnp.bfloat16


def round_up(value, unit):
    return -(-value // unit) * unit


def dot(a, b):
    return jnp.dot(a, b, preferred_element_type=F32)


def iota(shape, dim):
    return lax.broadcasted_iota(jnp.int32, shape, dim)


def rms_scale(widened, gain):
    return widened * lax.rsqrt(jnp.mean(widened * widened, axis=-1, keepdims=True) + EPSILON) * gain


def kernel(
    sizes,
    q_ref,
    kv_ref,
    key_gate_ref,
    mixw_ref,
    mix_gain_ref,
    x_ref,
    x_gain_ref,
    routes_t_ref,
    route_weight_t_ref,
    gate_hbm,
    up_hbm,
    down_hbm,
    mix_out,
    moe_out,
    gate_all,
    up_all,
    down_all,
    pick_all,
    normed_all,
    send_x,
    recv_x,
    hidden,
    send_y,
    recv_y,
    kv_all,
    q_pad,
    query_gate,
    top,
    total,
    summed,
    mix_send,
    mix_recv,
    local_sem,
    far_send,
    far_recv,
    own_send,
    own_recv,
    fwd_send,
    fwd_recv,
    x_send_sem,
    x_recv_sem,
    kv_send_sem,
    kv_recv_sem,
    y_send_sem,
    y_recv_sem,
    mix_send_sem,
    mix_recv_sem,
):
    ep, tp, slot_rows, wire_rows, chunks = sizes
    me = lax.axis_index("ep")
    tme = lax.axis_index("tp")
    far = lax.rem(tme + tp // 2, tp)
    near = tme + 1 - 2 * lax.rem(tme, 2)
    near_far = lax.rem(near + tp // 2, tp)
    rows, width = x_ref.shape
    picks = routes_t_ref.shape[0]
    slots = ep * slot_rows
    shard = down_hbm.shape[1]
    cols = width // chunks
    tokens = q_ref.shape[0]
    heads = key_gate_ref.shape[1]
    half = ep // 2
    own_start = (me // half) * half
    cross_start = half - own_start
    turn = me - own_start
    kv_local = kv_ref.shape[1] // (2 * HEAD)
    group = heads // kv_local

    def weight_view(item, block):
        if item == 0:
            return gate_all.at[block]
        if item == 1:
            return up_all.at[block]
        return down_all.at[item - 2, pl.ds(pl.multiple_of(block * shard, shard), shard)]

    def weight_source(item):
        if item == 0:
            return gate_hbm.at[0]
        if item == 1:
            return up_hbm.at[0]
        return down_hbm.at[0, :, pl.ds((item - 2) * cols, cols)]

    items = 2 + chunks
    loads = [
        pltpu.make_async_copy(weight_source(i), weight_view(i, tme), local_sem.at[i])
        for i in range(items)
    ]
    for load in loads:
        load.start()
    recv_x[...] = jnp.zeros_like(recv_x)
    recv_y[...] = jnp.zeros_like(recv_y)

    barrier = pltpu.get_barrier_semaphore()

    def greet(step, carry):
        pl.semaphore_signal(
            barrier, inc=1, device_id={"ep": lax.rem(me + step, ep)}, device_id_type=MESH
        )
        return carry

    lax.fori_loop(1, ep, greet, 0)
    for step in range(1, tp):
        pl.semaphore_signal(
            barrier, inc=1, device_id={"tp": lax.rem(tme + step, tp)}, device_id_type=MESH
        )
    normed = rms_scale(x_ref[...].astype(F32), x_gain_ref[...]).astype(BF16)
    expert_row = iota((ep, rows), 0)
    named_t = jnp.zeros((ep, rows), F32)
    for k in range(picks):
        named_t = named_t + jnp.where(routes_t_ref[k : k + 1, :] == expert_row, 1.0, 0.0)
    before_t = jnp.where(iota((rows, rows), 0) < iota((rows, rows), 1), 1.0, 0.0).astype(BF16)
    place_t = dot(named_t.astype(BF16), before_t) + (expert_row * slot_rows).astype(F32)
    slot_iota = iota((slots, rows), 0)
    pick_t = jnp.zeros((slots, rows), F32)
    slot_rows_of = []
    for k in range(picks):
        slot_t = jnp.sum(
            jnp.where(routes_t_ref[k : k + 1, :] == expert_row, place_t, 0.0), axis=0, keepdims=True
        )
        slot_rows_of.append(slot_t)
        pick_t = pick_t + jnp.where(slot_iota == slot_t.astype(jnp.int32), 1.0, 0.0)
    pick_all[...] = pick_t.astype(BF16).reshape(ep, slot_rows, rows)
    normed_all[...] = normed

    pl.semaphore_wait(barrier, ep - 1 + tp - 1)

    def weight_copy(item, block, target, send_sem, recv_sem):
        view = weight_view(item, block)
        return pltpu.make_async_remote_copy(
            src_ref=view,
            dst_ref=view,
            send_sem=send_sem.at[item],
            recv_sem=recv_sem.at[item],
            device_id={"tp": target},
            device_id_type=MESH,
        )

    far_copies, own_copies, fwd_copies = [], [], []
    for i in range(items):
        loads[i].wait()
        far_copies.append(weight_copy(i, tme, far, far_send, far_recv))
        far_copies[i].start()
        own_copies.append(weight_copy(i, tme, near, own_send, own_recv))
        own_copies[i].start()
        fwd_copies.append(weight_copy(i, far, near, fwd_send, fwd_recv))

    def far_arrival(item):
        return weight_copy(item, far, far, far_send, far_recv)

    def near_arrival(item):
        return weight_copy(item, near, near, own_send, own_recv)

    def near_far_arrival(item):
        return weight_copy(item, near_far, near, fwd_send, fwd_recv)

    def x_copy(target, source):
        return pltpu.make_async_remote_copy(
            src_ref=send_x.at[target, pl.ds(0, wire_rows)],
            dst_ref=recv_x.at[source, pl.ds(0, wire_rows)],
            send_sem=x_send_sem.at[target],
            recv_sem=x_recv_sem.at[source],
            device_id={"ep": target},
            device_id_type=MESH,
        )

    def kv_copy(target, source):
        return pltpu.make_async_remote_copy(
            src_ref=kv_ref,
            dst_ref=kv_all.at[source],
            send_sem=kv_send_sem.at[target],
            recv_sem=kv_recv_sem.at[source],
            device_id={"ep": target},
            device_id_type=MESH,
        )

    def over_peers(action):
        def step_of(step, carry):
            action(lax.rem(me + step, ep))
            return carry

        lax.fori_loop(1, ep, step_of, 0)

    def over_half(start, first, action):
        def step_of(step, carry):
            action(start + lax.rem(turn + step, half))
            return carry

        lax.fori_loop(first, half, step_of, 0)

    def fill(peer):
        return dot(pick_all[peer], normed_all[...]).astype(BF16)

    def dispatch(peer):
        send_x[peer] = fill(peer)
        x_copy(peer, me).start()

    def dispatch_pair(step, carry):
        dispatch(cross_start + lax.rem(turn + step, half))

        @pl.when(step > 0)
        def _():
            dispatch(own_start + lax.rem(turn + step, half))

        return carry

    lax.fori_loop(0, half, dispatch_pair, 0)

    def kv_start(peer, carry):
        kv_copy(peer, me).start()
        return carry

    lax.fori_loop(me + 1, ep, kv_start, 0)
    recv_x[me] = fill(me)
    kv_all[me] = kv_ref[...]

    def column(row):
        size = row.shape[1]
        same = iota((size, size), 0) == iota((size, size), 1)
        return jnp.sum(jnp.where(same, row, 0.0), axis=1, keepdims=True)

    slot_of = [column(row).astype(jnp.int32) for row in slot_rows_of]
    for h in range(heads):
        select = jnp.where(
            (iota((heads * HEAD, 2 * HEAD), 0) == iota((heads * HEAD, 2 * HEAD), 1) + h * HEAD)
            & (iota((heads * HEAD, 2 * HEAD), 1) < HEAD),
            1.0,
            0.0,
        ).astype(BF16)
        q_pad[h] = dot(q_ref[...], select).astype(BF16)
        query_gate[h] = column(key_gate_ref[me, h : h + 1, :])
    top[...] = jnp.full(top.shape, NEGATIVE, F32)
    total[...] = jnp.zeros_like(total)
    summed[...] = jnp.zeros_like(summed)

    for i in range(2):
        far_arrival(i).wait_recv()
        fwd_copies[i].start()
    for i in range(2):
        near_arrival(i).wait_recv()
        near_far_arrival(i).wait_recv()

    def hidden_half(start, index):
        def hidden_block(block, carry):
            taken = recv_x[pl.ds(start, half)].reshape(half * slot_rows, width)
            gated = dot(taken, gate_all[block])
            lifted = dot(taken, up_all[block])
            hidden[index, :, pl.ds(pl.multiple_of(block * shard, shard), shard)] = (
                gated / (1.0 + jnp.exp(-gated)) * lifted
            ).astype(BF16)
            return carry

        lax.fori_loop(0, tp, hidden_block, 0)

    over_half(own_start, 1, lambda peer: x_copy(me, peer).wait_recv())
    hidden_half(own_start, 0)
    far_arrival(2).wait_recv()
    fwd_copies[2].start()
    over_half(cross_start, 0, lambda peer: x_copy(me, peer).wait_recv())
    hidden_half(cross_start, 1)

    def y_copy(c, target, source):
        return pltpu.make_async_remote_copy(
            src_ref=send_y.at[c, target, pl.ds(0, wire_rows)],
            dst_ref=recv_y.at[c, source, pl.ds(0, wire_rows)],
            send_sem=y_send_sem.at[c, target],
            recv_sem=y_recv_sem.at[c, source],
            device_id={"ep": target},
            device_id_type=MESH,
        )

    def results(c, start, index):
        send_y[c, pl.ds(start, half)] = (
            dot(hidden[index], down_all[c]).astype(BF16).reshape(half, slot_rows, cols)
        )

    for c in range(chunks):
        if c > 0:
            far_arrival(2 + c).wait_recv()
            fwd_copies[2 + c].start()
        near_arrival(2 + c).wait_recv()
        near_far_arrival(2 + c).wait_recv()
        results(c, cross_start, 1)
        over_half(cross_start, 0, lambda peer: y_copy(c, peer, me).start())
    for c in range(chunks):
        results(c, own_start, 0)
        over_half(own_start, 1, lambda peer: y_copy(c, peer, me).start())
        recv_y[c, me] = send_y[c, me]

    def key_block(block, carry):
        @pl.when(block < me)
        def _():
            kv_copy(me, block).wait_recv()

        causal = block * tokens + iota((tokens, tokens), 1) <= me * tokens + iota(
            (tokens, tokens), 0
        )
        for h in range(heads):
            pair = kv_all[block, :, (h // group) * 2 * HEAD : (h // group + 1) * 2 * HEAD]
            scores = (
                lax.dot_general(
                    q_pad[h], pair, (((1,), (1,)), ((), ())), preferred_element_type=F32
                )
                * HEAD ** (-0.5)
            )
            scores = scores + query_gate[h] - key_gate_ref[block, h : h + 1, :]
            scores = jnp.where(causal, scores, NEGATIVE)
            old = top[h]
            new = jnp.maximum(old, jnp.max(scores, axis=-1, keepdims=True))
            factor = jnp.exp(old - new)
            weight = jnp.where(causal, jnp.exp(scores - new[:, :1]), 0.0)
            top[h] = new
            total[h] = total[h] * factor + jnp.sum(weight, axis=-1, keepdims=True)
            summed[h] = summed[h] * factor + dot(weight.astype(BF16), pair)
        return carry

    lax.fori_loop(0, me + 1, key_block, 0)
    attended = jnp.zeros((tokens, heads * HEAD), F32)
    for h in range(heads):
        part = (summed[h] / total[h]).astype(BF16)
        select = jnp.where(
            (iota((2 * HEAD, heads * HEAD), 0) + (h - 1) * HEAD == iota((2 * HEAD, heads * HEAD), 1))
            & (iota((2 * HEAD, heads * HEAD), 0) >= HEAD),
            1.0,
            0.0,
        ).astype(BF16)
        attended = attended + dot(part, select)
    attended = attended.astype(BF16)
    for c in range(chunks):
        mix_send[:, :, c * cols : (c + 1) * cols] = (
            dot(attended, mixw_ref[:, c * cols : (c + 1) * cols])
            .astype(BF16)
            .reshape(tp, tokens // tp, cols)
        )

    def mix_copy(target, source):
        return pltpu.make_async_remote_copy(
            src_ref=mix_send.at[target],
            dst_ref=mix_recv.at[source],
            send_sem=mix_send_sem.at[target],
            recv_sem=mix_recv_sem.at[source],
            device_id={"tp": target},
            device_id_type=MESH,
        )

    for step in range(1, tp):
        mix_copy(lax.rem(tme + step, tp), tme).start()
    mix_recv[tme] = mix_send[tme]
    for step in range(1, tp):
        mix_copy(tme, lax.rem(tme + step, tp)).wait_recv()
    mixed = mix_recv[0].astype(F32)
    for j in range(1, tp):
        mixed = mixed + mix_recv[j].astype(F32)
    mix_out[...] = rms_scale(mixed, mix_gain_ref[...]).astype(BF16)

    slot_lane = iota((rows, slots), 1)
    scale_of = [column(route_weight_t_ref[k : k + 1, :]) for k in range(picks)]
    for c in range(chunks):
        over_peers(lambda peer: y_copy(c, me, peer).wait_recv())
        back = recv_y[c].reshape(slots, cols)
        blend = jnp.zeros((rows, cols), F32)
        for k in range(picks):
            pick = jnp.where(slot_lane == slot_of[k], 1.0, 0.0).astype(BF16)
            blend = blend + scale_of[k] * dot(pick, back)
        moe_out[:, c * cols : (c + 1) * cols] = blend.astype(BF16)

    for i in range(items):
        far_copies[i].wait_send()
        own_copies[i].wait_send()
        fwd_copies[i].wait_send()
    over_peers(lambda peer: x_copy(peer, me).wait_send())

    def kv_end(peer, carry):
        kv_copy(peer, me).wait_send()
        return carry

    lax.fori_loop(me + 1, ep, kv_end, 0)
    for c in range(chunks):
        over_peers(lambda peer: y_copy(c, peer, me).wait_send())
    for step in range(1, tp):
        mix_copy(lax.rem(tme + step, tp), tme).wait_send()


def copy_kernel(mix_in, moe_in, mix_out, moe_out):
    mix_out[...] = mix_in[...]
    moe_out[...] = moe_in[...]


def body(
    queries,
    keys_values,
    log_gate_cum,
    mix_weight,
    mix_gain,
    moe_in,
    moe_gain,
    routes,
    route_weight,
    expert_gate,
    expert_up,
    expert_down,
):
    ep, tp = lax.axis_size("ep"), lax.axis_size("tp")
    tokens = queries.shape[0]
    heads = log_gate_cum.shape[0]
    rows, width = moe_in.shape
    picks = routes.shape[1]
    capacity = 3 * picks * rows // (2 * ep)
    slot_rows, wire_rows = round_up(capacity, 16), round_up(capacity, WIRE)
    chunks = 4
    cols = width // chunks
    depth, shard = expert_gate.shape[1:]
    key_gate = jnp.transpose(log_gate_cum.reshape(heads, ep, tokens), (1, 0, 2))
    vmem = pl.BlockSpec(memory_space=pltpu.VMEM)
    hbm = pl.BlockSpec(memory_space=pl.ANY)
    dma = pltpu.SemaphoreType.DMA
    items = 2 + chunks
    results = pl.pallas_call(
        partial(kernel, (ep, tp, slot_rows, wire_rows, chunks)),
        out_shape=(
            jax.ShapeDtypeStruct((tokens // tp, width), BF16),
            jax.ShapeDtypeStruct((rows, width), BF16),
        ),
        in_specs=[vmem] * 9 + [hbm] * 3,
        out_specs=(vmem, vmem),
        scratch_shapes=[
            pltpu.VMEM((tp, depth, shard), BF16),
            pltpu.VMEM((tp, depth, shard), BF16),
            pltpu.VMEM((chunks, tp * shard, cols), BF16),
            pltpu.VMEM((ep, slot_rows, rows), BF16),
            pltpu.VMEM((rows, width), BF16),
            pltpu.VMEM((ep, slot_rows, width), BF16),
            pltpu.VMEM((ep, slot_rows, width), BF16),
            pltpu.VMEM((2, ep // 2 * slot_rows, tp * shard), BF16),
            pltpu.VMEM((chunks, ep, slot_rows, cols), BF16),
            pltpu.VMEM((chunks, ep, slot_rows, cols), BF16),
            pltpu.VMEM((ep,) + keys_values.shape, BF16),
            pltpu.VMEM((heads, tokens, 2 * HEAD), BF16),
            pltpu.VMEM((heads, tokens, 1), F32),
            pltpu.VMEM((heads, tokens, 2 * HEAD), F32),
            pltpu.VMEM((heads, tokens, 2 * HEAD), F32),
            pltpu.VMEM((heads, tokens, 2 * HEAD), F32),
            pltpu.VMEM((tp, tokens // tp, width), BF16),
            pltpu.VMEM((tp, tokens // tp, width), BF16),
        ]
        + [dma((items,))] * 7
        + [dma((ep,))] * 4
        + [dma((chunks, ep))] * 2
        + [dma((tp,))] * 2,
        compiler_params=pltpu.CompilerParams(
            collective_id=0, has_side_effects=True, vmem_limit_bytes=60 * 1024 * 1024
        ),
    )(
        queries,
        keys_values,
        key_gate,
        mix_weight,
        mix_gain.reshape(1, -1),
        moe_in,
        moe_gain.reshape(1, -1),
        routes.T,
        route_weight.T,
        expert_gate,
        expert_up,
        expert_down,
    )

    return pl.pallas_call(
        copy_kernel,
        out_shape=tuple(jax.ShapeDtypeStruct(r.shape, r.dtype) for r in results),
        in_specs=[vmem] * 2,
        out_specs=(vmem, vmem),
    )(*results)


WIRE = 8


def solution(mesh):
    in_specs = (
        P("ep", "tp"),
        P("ep", "tp"),
        P("tp", None),
        P("tp", None),
        P(),
        P(("ep", "tp"), None),
        P(),
        P(("ep", "tp"), None),
        P(("ep", "tp"), None),
        P("ep", None, "tp"),
        P("ep", None, "tp"),
        P("ep", "tp", None),
    )
    out_specs = (P(("ep", "tp"), None), P(("ep", "tp"), None))
    return jax.shard_map(body, mesh=mesh, in_specs=in_specs, out_specs=out_specs, check_vma=False)
```

```python
from functools import partial

import jax
import jax.numpy as jnp
from jax import lax
from jax.experimental import pallas as pl
from jax.experimental.pallas import tpu as pltpu
from jax.sharding import PartitionSpec as P

HEAD = 64
EPSILON = 1e-06
NEGATIVE = -1e30
MESH = pl.DeviceIdType.MESH
F32 = jnp.float32
BF16 = jnp.bfloat16


def round_up(value, unit):
    return -(-value // unit) * unit


def dot(a, b):
    return jnp.dot(a, b, preferred_element_type=F32)


def iota(shape, dim):
    return lax.broadcasted_iota(jnp.int32, shape, dim)


def rms_scale(widened, gain):
    return widened * lax.rsqrt(jnp.mean(widened * widened, axis=-1, keepdims=True) + EPSILON) * gain


def kernel(
    sizes,
    q_ref,
    kv_ref,
    key_gate_ref,
    mixw_ref,
    mix_gain_ref,
    x_ref,
    x_gain_ref,
    routes_t_ref,
    route_weight_t_ref,
    gate_hbm,
    up_hbm,
    down_hbm,
    mix_out,
    moe_out,
    gate_all,
    up_all,
    down_all,
    pick_all,
    normed_all,
    send_x,
    recv_x,
    hidden,
    send_y,
    recv_y,
    kv_all,
    q_pad,
    query_gate,
    top,
    total,
    summed,
    mix_send,
    mix_recv,
    local_sem,
    far_send,
    far_recv,
    own_send,
    own_recv,
    fwd_send,
    fwd_recv,
    x_send_sem,
    x_recv_sem,
    kv_send_sem,
    kv_recv_sem,
    y_send_sem,
    y_recv_sem,
    mix_send_sem,
    mix_recv_sem,
):
    ep, tp, slot_rows, wire_rows, chunks = sizes
    me = lax.axis_index("ep")
    tme = lax.axis_index("tp")
    far = lax.rem(tme + tp // 2, tp)
    near = tme + 1 - 2 * lax.rem(tme, 2)
    near_far = lax.rem(near + tp // 2, tp)
    rows, width = x_ref.shape
    picks = routes_t_ref.shape[0]
    slots = ep * slot_rows
    shard = down_hbm.shape[1]
    cols = width // chunks
    tokens = q_ref.shape[0]
    heads = key_gate_ref.shape[1]
    half = ep // 2
    own_start = (me // half) * half
    cross_start = half - own_start
    turn = me - own_start
    kv_local = kv_ref.shape[1] // (2 * HEAD)
    group = heads // kv_local

    def weight_view(item, block):
        if item == 0:
            return gate_all.at[block]
        if item == 1:
            return up_all.at[block]
        return down_all.at[item - 2, pl.ds(pl.multiple_of(block * shard, shard), shard)]

    def weight_source(item):
        if item == 0:
            return gate_hbm.at[0]
        if item == 1:
            return up_hbm.at[0]
        return down_hbm.at[0, :, pl.ds((item - 2) * cols, cols)]

    items = 2 + chunks
    loads = [
        pltpu.make_async_copy(weight_source(i), weight_view(i, tme), local_sem.at[i])
        for i in range(items)
    ]
    for load in loads:
        load.start()
    recv_x[...] = jnp.zeros_like(recv_x)
    recv_y[...] = jnp.zeros_like(recv_y)

    barrier = pltpu.get_barrier_semaphore()

    def greet(step, carry):
        pl.semaphore_signal(
            barrier, inc=1, device_id={"ep": lax.rem(me + step, ep)}, device_id_type=MESH
        )
        return carry

    lax.fori_loop(1, ep, greet, 0)
    for step in range(1, tp):
        pl.semaphore_signal(
            barrier, inc=1, device_id={"tp": lax.rem(tme + step, tp)}, device_id_type=MESH
        )
    normed = rms_scale(x_ref[...].astype(F32), x_gain_ref[...]).astype(BF16)
    expert_row = iota((ep, rows), 0)
    named_t = jnp.zeros((ep, rows), F32)
    for k in range(picks):
        named_t = named_t + jnp.where(routes_t_ref[k : k + 1, :] == expert_row, 1.0, 0.0)
    before_t = jnp.where(iota((rows, rows), 0) < iota((rows, rows), 1), 1.0, 0.0).astype(BF16)
    place_t = dot(named_t.astype(BF16), before_t) + (expert_row * slot_rows).astype(F32)
    slot_iota = iota((slots, rows), 0)
    pick_t = jnp.zeros((slots, rows), F32)
    slot_rows_of = []
    for k in range(picks):
        slot_t = jnp.sum(
            jnp.where(routes_t_ref[k : k + 1, :] == expert_row, place_t, 0.0), axis=0, keepdims=True
        )
        slot_rows_of.append(slot_t)
        pick_t = pick_t + jnp.where(slot_iota == slot_t.astype(jnp.int32), 1.0, 0.0)
    pick_all[...] = pick_t.astype(BF16).reshape(ep, slot_rows, rows)
    normed_all[...] = normed

    pl.semaphore_wait(barrier, ep - 1 + tp - 1)

    def weight_copy(item, block, target, send_sem, recv_sem):
        view = weight_view(item, block)
        return pltpu.make_async_remote_copy(
            src_ref=view,
            dst_ref=view,
            send_sem=send_sem.at[item],
            recv_sem=recv_sem.at[item],
            device_id={"tp": target},
            device_id_type=MESH,
        )

    far_copies, own_copies, fwd_copies = [], [], []
    for i in range(items):
        loads[i].wait()
        far_copies.append(weight_copy(i, tme, far, far_send, far_recv))
        far_copies[i].start()
        own_copies.append(weight_copy(i, tme, near, own_send, own_recv))
        own_copies[i].start()
        fwd_copies.append(weight_copy(i, far, near, fwd_send, fwd_recv))

    def far_arrival(item):
        return weight_copy(item, far, far, far_send, far_recv)

    def near_arrival(item):
        return weight_copy(item, near, near, own_send, own_recv)

    def near_far_arrival(item):
        return weight_copy(item, near_far, near, fwd_send, fwd_recv)

    def x_copy(target, source):
        return pltpu.make_async_remote_copy(
            src_ref=send_x.at[target, pl.ds(0, wire_rows)],
            dst_ref=recv_x.at[source, pl.ds(0, wire_rows)],
            send_sem=x_send_sem.at[target],
            recv_sem=x_recv_sem.at[source],
            device_id={"ep": target},
            device_id_type=MESH,
        )

    def kv_copy(target, source):
        return pltpu.make_async_remote_copy(
            src_ref=kv_ref,
            dst_ref=kv_all.at[source],
            send_sem=kv_send_sem.at[target],
            recv_sem=kv_recv_sem.at[source],
            device_id={"ep": target},
            device_id_type=MESH,
        )

    def over_peers(action):
        def step_of(step, carry):
            action(lax.rem(me + step, ep))
            return carry

        lax.fori_loop(1, ep, step_of, 0)

    def over_half(start, first, action):
        def step_of(step, carry):
            action(start + lax.rem(turn + step, half))
            return carry

        lax.fori_loop(first, half, step_of, 0)

    def fill(peer):
        return dot(pick_all[peer], normed_all[...]).astype(BF16)

    def dispatch(peer):
        send_x[peer] = fill(peer)
        x_copy(peer, me).start()

    def dispatch_pair(step, carry):
        dispatch(cross_start + lax.rem(turn + step, half))

        @pl.when(step > 0)
        def _():
            dispatch(own_start + lax.rem(turn + step, half))

        return carry

    lax.fori_loop(0, half, dispatch_pair, 0)

    def kv_start(peer, carry):
        kv_copy(peer, me).start()
        return carry

    lax.fori_loop(me + 1, ep, kv_start, 0)
    recv_x[me] = fill(me)
    kv_all[me] = kv_ref[...]

    def column(row):
        size = row.shape[1]
        same = iota((size, size), 0) == iota((size, size), 1)
        return jnp.sum(jnp.where(same, row, 0.0), axis=1, keepdims=True)

    slot_of = [column(row).astype(jnp.int32) for row in slot_rows_of]
    for h in range(heads):
        select = jnp.where(
            (iota((heads * HEAD, 2 * HEAD), 0) == iota((heads * HEAD, 2 * HEAD), 1) + h * HEAD)
            & (iota((heads * HEAD, 2 * HEAD), 1) < HEAD),
            1.0,
            0.0,
        ).astype(BF16)
        q_pad[h] = dot(q_ref[...], select).astype(BF16)
        query_gate[h] = column(key_gate_ref[me, h : h + 1, :])
    top[...] = jnp.full(top.shape, NEGATIVE, F32)
    total[...] = jnp.zeros_like(total)
    summed[...] = jnp.zeros_like(summed)

    for i in range(2):
        far_arrival(i).wait_recv()
        fwd_copies[i].start()
    for i in range(2):
        near_arrival(i).wait_recv()
        near_far_arrival(i).wait_recv()

    def hidden_half(start, index):
        def hidden_block(block, carry):
            taken = recv_x[pl.ds(start, half)].reshape(half * slot_rows, width)
            gated = dot(taken, gate_all[block])
            lifted = dot(taken, up_all[block])
            hidden[index, :, pl.ds(pl.multiple_of(block * shard, shard), shard)] = (
                gated / (1.0 + jnp.exp(-gated)) * lifted
            ).astype(BF16)
            return carry

        lax.fori_loop(0, tp, hidden_block, 0)

    over_half(own_start, 1, lambda peer: x_copy(me, peer).wait_recv())
    hidden_half(own_start, 0)
    far_arrival(2).wait_recv()
    fwd_copies[2].start()
    over_half(cross_start, 0, lambda peer: x_copy(me, peer).wait_recv())
    hidden_half(cross_start, 1)

    def y_copy(c, target, source):
        return pltpu.make_async_remote_copy(
            src_ref=send_y.at[c, target, pl.ds(0, wire_rows)],
            dst_ref=recv_y.at[c, source, pl.ds(0, wire_rows)],
            send_sem=y_send_sem.at[c, target],
            recv_sem=y_recv_sem.at[c, source],
            device_id={"ep": target},
            device_id_type=MESH,
        )

    def results(c, start, index):
        send_y[c, pl.ds(start, half)] = (
            dot(hidden[index], down_all[c]).astype(BF16).reshape(half, slot_rows, cols)
        )

    for c in range(chunks):
        if c > 0:
            far_arrival(2 + c).wait_recv()
            fwd_copies[2 + c].start()
        near_arrival(2 + c).wait_recv()
        near_far_arrival(2 + c).wait_recv()
        results(c, cross_start, 1)
        over_half(cross_start, 0, lambda peer: y_copy(c, peer, me).start())
    for c in range(chunks):
        results(c, own_start, 0)
        over_half(own_start, 1, lambda peer: y_copy(c, peer, me).start())
        recv_y[c, me] = send_y[c, me]

    def key_block(block, carry):
        @pl.when(block < me)
        def _():
            kv_copy(me, block).wait_recv()

        causal = block * tokens + iota((tokens, tokens), 1) <= me * tokens + iota(
            (tokens, tokens), 0
        )
        for h in range(heads):
            pair = kv_all[block, :, (h // group) * 2 * HEAD : (h // group + 1) * 2 * HEAD]
            scores = (
                lax.dot_general(
                    q_pad[h], pair, (((1,), (1,)), ((), ())), preferred_element_type=F32
                )
                * HEAD ** (-0.5)
            )
            scores = scores + query_gate[h] - key_gate_ref[block, h : h + 1, :]
            scores = jnp.where(causal, scores, NEGATIVE)
            old = top[h]
            new = jnp.maximum(old, jnp.max(scores, axis=-1, keepdims=True))
            factor = jnp.exp(old - new)
            weight = jnp.where(causal, jnp.exp(scores - new[:, :1]), 0.0)
            top[h] = new
            total[h] = total[h] * factor + jnp.sum(weight, axis=-1, keepdims=True)
            summed[h] = summed[h] * factor + dot(weight.astype(BF16), pair)
        return carry

    lax.fori_loop(0, me + 1, key_block, 0)
    attended = jnp.zeros((tokens, heads * HEAD), F32)
    for h in range(heads):
        part = (summed[h] / total[h]).astype(BF16)
        select = jnp.where(
            (iota((2 * HEAD, heads * HEAD), 0) + (h - 1) * HEAD == iota((2 * HEAD, heads * HEAD), 1))
            & (iota((2 * HEAD, heads * HEAD), 0) >= HEAD),
            1.0,
            0.0,
        ).astype(BF16)
        attended = attended + dot(part, select)
    attended = attended.astype(BF16)
    for c in range(chunks):
        mix_send[:, :, c * cols : (c + 1) * cols] = (
            dot(attended, mixw_ref[:, c * cols : (c + 1) * cols])
            .astype(BF16)
            .reshape(tp, tokens // tp, cols)
        )

    def mix_copy(target, source):
        return pltpu.make_async_remote_copy(
            src_ref=mix_send.at[target],
            dst_ref=mix_recv.at[source],
            send_sem=mix_send_sem.at[target],
            recv_sem=mix_recv_sem.at[source],
            device_id={"tp": target},
            device_id_type=MESH,
        )

    for step in range(1, tp):
        mix_copy(lax.rem(tme + step, tp), tme).start()
    mix_recv[tme] = mix_send[tme]
    for step in range(1, tp):
        mix_copy(tme, lax.rem(tme + step, tp)).wait_recv()
    mixed = mix_recv[0].astype(F32)
    for j in range(1, tp):
        mixed = mixed + mix_recv[j].astype(F32)
    mix_out[...] = rms_scale(mixed, mix_gain_ref[...]).astype(BF16)

    slot_lane = iota((rows, slots), 1)
    scale_of = [column(route_weight_t_ref[k : k + 1, :]) for k in range(picks)]
    for c in range(chunks):
        over_peers(lambda peer: y_copy(c, me, peer).wait_recv())
        back = recv_y[c].reshape(slots, cols)
        blend = jnp.zeros((rows, cols), F32)
        for k in range(picks):
            pick = jnp.where(slot_lane == slot_of[k], 1.0, 0.0).astype(BF16)
            blend = blend + scale_of[k] * dot(pick, back)
        moe_out[:, c * cols : (c + 1) * cols] = blend.astype(BF16)

    for i in range(items):
        far_copies[i].wait_send()
        own_copies[i].wait_send()
        fwd_copies[i].wait_send()
    over_peers(lambda peer: x_copy(peer, me).wait_send())

    def kv_end(peer, carry):
        kv_copy(peer, me).wait_send()
        return carry

    lax.fori_loop(me + 1, ep, kv_end, 0)
    for c in range(chunks):
        over_peers(lambda peer: y_copy(c, peer, me).wait_send())
    for step in range(1, tp):
        mix_copy(lax.rem(tme + step, tp), tme).wait_send()


def copy_kernel(mix_in, moe_in, mix_out, moe_out):
    mix_out[...] = mix_in[...]
    moe_out[...] = moe_in[...]


def body(
    queries,
    keys_values,
    log_gate_cum,
    mix_weight,
    mix_gain,
    moe_in,
    moe_gain,
    routes,
    route_weight,
    expert_gate,
    expert_up,
    expert_down,
):
    ep, tp = lax.axis_size("ep"), lax.axis_size("tp")
    tokens = queries.shape[0]
    heads = log_gate_cum.shape[0]
    rows, width = moe_in.shape
    picks = routes.shape[1]
    capacity = 3 * picks * rows // (2 * ep)
    slot_rows, wire_rows = round_up(capacity, 16), round_up(capacity, WIRE)
    chunks = 8
    cols = width // chunks
    depth, shard = expert_gate.shape[1:]
    key_gate = jnp.transpose(log_gate_cum.reshape(heads, ep, tokens), (1, 0, 2))
    vmem = pl.BlockSpec(memory_space=pltpu.VMEM)
    hbm = pl.BlockSpec(memory_space=pl.ANY)
    dma = pltpu.SemaphoreType.DMA
    items = 2 + chunks
    results = pl.pallas_call(
        partial(kernel, (ep, tp, slot_rows, wire_rows, chunks)),
        out_shape=(
            jax.ShapeDtypeStruct((tokens // tp, width), BF16),
            jax.ShapeDtypeStruct((rows, width), BF16),
        ),
        in_specs=[vmem] * 9 + [hbm] * 3,
        out_specs=(vmem, vmem),
        scratch_shapes=[
            pltpu.VMEM((tp, depth, shard), BF16),
            pltpu.VMEM((tp, depth, shard), BF16),
            pltpu.VMEM((chunks, tp * shard, cols), BF16),
            pltpu.VMEM((ep, slot_rows, rows), BF16),
            pltpu.VMEM((rows, width), BF16),
            pltpu.VMEM((ep, slot_rows, width), BF16),
            pltpu.VMEM((ep, slot_rows, width), BF16),
            pltpu.VMEM((2, ep // 2 * slot_rows, tp * shard), BF16),
            pltpu.VMEM((chunks, ep, slot_rows, cols), BF16),
            pltpu.VMEM((chunks, ep, slot_rows, cols), BF16),
            pltpu.VMEM((ep,) + keys_values.shape, BF16),
            pltpu.VMEM((heads, tokens, 2 * HEAD), BF16),
            pltpu.VMEM((heads, tokens, 1), F32),
            pltpu.VMEM((heads, tokens, 2 * HEAD), F32),
            pltpu.VMEM((heads, tokens, 2 * HEAD), F32),
            pltpu.VMEM((heads, tokens, 2 * HEAD), F32),
            pltpu.VMEM((tp, tokens // tp, width), BF16),
            pltpu.VMEM((tp, tokens // tp, width), BF16),
        ]
        + [dma((items,))] * 7
        + [dma((ep,))] * 4
        + [dma((chunks, ep))] * 2
        + [dma((tp,))] * 2,
        compiler_params=pltpu.CompilerParams(
            collective_id=0, has_side_effects=True, vmem_limit_bytes=60 * 1024 * 1024
        ),
    )(
        queries,
        keys_values,
        key_gate,
        mix_weight,
        mix_gain.reshape(1, -1),
        moe_in,
        moe_gain.reshape(1, -1),
        routes.T,
        route_weight.T,
        expert_gate,
        expert_up,
        expert_down,
    )

    return pl.pallas_call(
        copy_kernel,
        out_shape=tuple(jax.ShapeDtypeStruct(r.shape, r.dtype) for r in results),
        in_specs=[vmem] * 2,
        out_specs=(vmem, vmem),
    )(*results)


WIRE = 8


def solution(mesh):
    in_specs = (
        P("ep", "tp"),
        P("ep", "tp"),
        P("tp", None),
        P("tp", None),
        P(),
        P(("ep", "tp"), None),
        P(),
        P(("ep", "tp"), None),
        P(("ep", "tp"), None),
        P("ep", None, "tp"),
        P("ep", None, "tp"),
        P("ep", "tp", None),
    )
    out_specs = (P(("ep", "tp"), None), P(("ep", "tp"), None))
    return jax.shard_map(body, mesh=mesh, in_specs=in_specs, out_specs=out_specs, check_vma=False)
```
